512 devices in a mesh: grp: 2 (over y), fs: 32 (over z), tp: 8 (over x, core).
Axes of the slice: x: 4, y: 2, z: 32, core: 2. Of those that a mesh axis runs over, the one named last changes fastest.
The devices are a block of a 4x8x32 slice.
Arguments:
- stream: bfloat16 [64, 128, 2048], P(('grp', 'fs')), parts along dimension 0, may hold values from -6 to 6
- in_gain: float32 [2048], replicated, may hold values from 0.2 to 5
- value_weight: bfloat16 [2048, 1024], P('fs', 'tp'), may hold values from -0.125 to 0.125
- gate_weight: bfloat16 [2048, 1024], P('fs', 'tp'), may hold values from -0.125 to 0.125
- conv_kernel: bfloat16 [31, 1024], P(None, 'tp'), may hold values from -3.6 to 3.6
- conv_gain: float32 [1024], P('tp'), may hold values from 0.1 to 1.9
- conv_shift: float32 [1024], P('tp'), may hold values from -3 to 3
- out_weight: bfloat16 [1024, 2048], P('tp', 'fs'), may hold values from -0.1875 to 0.1875
- norm_gain: float32 [2048], replicated, may hold values from 0.2 to 5
- up_weight: bfloat16 [2048, 8192], P('fs', 'tp'), may hold values from -0.125 to 0.125
- down_weight: bfloat16 [8192, 2048], P('tp', 'fs'), may hold values from -0.0625 to 0.0625
- out_gain: float32 [2048], P('tp'), may hold values from 0.1 to 1.9
Outputs:
- result: bfloat16 [64, 128, 2048], P(('grp', 'fs'), None, 'tp'), parts along dimension 0
The draws below stay inside these ranges and needn't reach their ends.
There are 2 independent parts, one for each index of `grp`. The reference program is written for one: setup_inputs(seed, part) draws one part's arguments, and reference() takes and returns one part's arrays. A program takes and returns all parts, laid end to end along the dimension named above; an argument that names none is the same for every part. Nothing has to cross between parts.
All inputs are finite; a program needn't handle non-finite values.
Results may differ from the reference program's by a relative error of at most 0.02.
Values may be sent and summed in bfloat16 or wider, within the bound.
No kernel may reach another device: no remote copies, remote signals or barrier semaphores. Data moves between devices by JAX's collectives and lax.ppermute only.
A program may use at most 64 MiB of HBM per device.

```python
import jax
import jax.numpy as jnp
from jax import lax

D = 2048
DC = 1024
FF = 8192
KW = 31
SEQ_LEN = 128
SEQS = 32
N_TP = 8


def rising(key, length_count, span):
    spread_at = jnp.arange(length_count, dtype=jnp.float32) / (length_count - 1) * 2.0 - 1.0
    baseline = 10.0 ** (span * spread_at)
    roughness = jax.random.uniform(key, (length_count,), jnp.float32, 0.8, 1.25)
    return baseline * roughness


def draw_in_gain(key, part):
    return rising(jax.random.fold_in(key, 11), D, 0.45).astype(jnp.float32)


def draw_norm_gain(key, part):
    return rising(jax.random.fold_in(key, 23), D, 0.45).astype(jnp.float32)


def draw_conv_kernel(key, part):
    inner = jax.random.fold_in(key, 37)
    taps = jnp.clip(jax.random.normal(inner, (KW, DC), jnp.float32), -4.0, 4.0)
    scales = rising(jax.random.fold_in(key, 41), DC, 0.45)
    return (taps * KW ** (-0.5) * scales[None, :]).astype(jnp.bfloat16)


def block_levels(rng, extent, cuts, least, top_value):
    loudness, own = 1.0, jax.random.fold_in(rng, 6)
    for position, parts in cuts:
        heights = jnp.exp(jax.random.uniform(jax.random.fold_in(own, position), (parts,), jnp.float32, least / len(cuts), top_value / len(cuts)))
        loudness = loudness * jnp.repeat(heights, extent[position] // parts).reshape([-1 if axis == position else 1 for axis in range(len(extent))])
    return loudness


def gaussian(key, extent, deviation, limit, pieces=(), held_as=jnp.bfloat16):
    values = jax.random.normal(key, extent, jnp.float32) * deviation
    if len(pieces) > 0:
        values = block_levels(key, extent, pieces, -0.22, 0.18) * values
    return jnp.clip(values, min=-limit, max=limit).astype(held_as)


def setup_inputs(seed: int = 0, part: int = 0) -> dict:
    streams_of = jax.random.split(jax.random.key(seed), 13)
    part_keys = jax.random.split(jax.random.fold_in(streams_of[12], part), 13)
    return {
        "stream": gaussian(part_keys[0], (SEQS, SEQ_LEN, D), 1.0, 6.0, ((0, 32),)),
        "in_gain": draw_in_gain(jax.random.fold_in(streams_of[12], 71), part),
        "value_weight": gaussian(streams_of[2], (D, DC), D ** -0.5, 0.125, ((0, 32), (1, 8))),
        "gate_weight": gaussian(streams_of[3], (D, DC), D ** -0.5, 0.125, ((0, 32), (1, 8))),
        "conv_kernel": draw_conv_kernel(jax.random.fold_in(streams_of[12], 71), part),
        "conv_gain": jnp.clip(1.0 + 0.18 * jax.random.normal(streams_of[5], (DC,), jnp.float32), 0.1, 1.9),
        "conv_shift": gaussian(streams_of[6], (DC,), 0.5, 3.0, ((0, 8),), jnp.float32),
        "out_weight": gaussian(streams_of[7], (DC, D), DC ** -0.5, 0.1875, ((0, 8), (1, 32))),
        "norm_gain": draw_norm_gain(jax.random.fold_in(streams_of[12], 71), part),
        "up_weight": gaussian(streams_of[9], (D, FF), D ** -0.5, 0.125, ((0, 32), (1, 8))),
        "down_weight": gaussian(streams_of[10], (FF, D), FF ** -0.5, 0.0625, ((0, 8), (1, 32))),
        "out_gain": jnp.clip(1.0 + 0.18 * jax.random.normal(streams_of[11], (D,), jnp.float32), 0.1, 1.9),
    }


norm_epsilon = 1e-05
residual_scale = 2.0 ** 0.25

def layer_norm(values, gain_vector):
    row_mean = lax.optimization_barrier(jnp.mean(values, axis=-1, keepdims=True))
    row_var = lax.optimization_barrier(jnp.mean(jnp.square(values - row_mean), axis=-1, keepdims=True))
    return (values - row_mean) * lax.rsqrt(row_var + norm_epsilon) * gain_vector

def grouped_product(left, right, groups):
    width = left.shape[1] // groups
    accum = jnp.zeros((left.shape[0], right.shape[1]), jnp.float32)
    for group_index in range(groups):
        partial_value = jnp.dot(left[:, group_index * width:(group_index + 1) * width], right[group_index * width:(group_index + 1) * width], preferred_element_type=jnp.float32).astype(jnp.bfloat16)
        partial_value = lax.optimization_barrier(partial_value)
        accum = accum + partial_value.astype(jnp.float32)
    return accum.astype(jnp.bfloat16)

def reference(stream, in_gain, value_weight, gate_weight, conv_kernel, conv_gain, conv_shift, out_weight, norm_gain, up_weight, down_weight, out_gain):
    seq_count, seq_length, model_width = stream.shape
    token_count = seq_count * seq_length
    stream_rows = stream.reshape(token_count, model_width).astype(jnp.float32)
    normed = layer_norm(stream_rows, in_gain).astype(jnp.bfloat16)
    values = jnp.dot(normed, value_weight, preferred_element_type=jnp.float32)
    gating = jnp.dot(normed, gate_weight, preferred_element_type=jnp.float32)
    gated = (values * jax.nn.sigmoid(gating)).astype(jnp.bfloat16)
    channels = gated.shape[1]
    convolved = lax.conv_general_dilated(gated.reshape(seq_count, seq_length, channels), conv_kernel[:, None, :], window_strides=(1,), padding=[(KW - 1, 0)], dimension_numbers=('NWC', 'WIO', 'NWC'), feature_group_count=channels, preferred_element_type=jnp.float32).reshape(token_count, channels)
    activated = jax.nn.silu(layer_norm(convolved, conv_gain) + conv_shift).astype(jnp.bfloat16)
    mixed = grouped_product(activated, out_weight, N_TP)
    settled = layer_norm(residual_scale * normed.astype(jnp.float32) + mixed.astype(jnp.float32), norm_gain).astype(jnp.bfloat16)
    hidden = jnp.square(jax.nn.relu(jnp.dot(settled, up_weight, preferred_element_type=jnp.float32))).astype(jnp.bfloat16)
    fed = grouped_product(hidden, down_weight, N_TP)
    result = layer_norm(residual_scale * settled.astype(jnp.float32) + fed.astype(jnp.float32), out_gain)
    return result.astype(jnp.bfloat16).reshape(seq_count, seq_length, model_width)
```

```python
import jax
import jax.numpy as jnp
from jax import lax
from jax.sharding import PartitionSpec as P

KW = 31

norm_epsilon = 1e-05
residual_scale = 2.0**0.25


def gather_fs(x):
    groups = lax.axis_size("grp")
    rows = x.shape[0] // groups
    own = lax.dynamic_slice_in_dim(x, lax.axis_index("grp") * rows, rows, 0)
    return lax.all_gather(own, ("fs", "grp"), axis=0, tiled=True)


def norm_rows(values, gain_vector):
    row_mean = jnp.mean(values, axis=-1, keepdims=True)
    row_var = jnp.mean(jnp.square(values - row_mean), axis=-1, keepdims=True)
    return (values - row_mean) * lax.rsqrt(row_var + norm_epsilon) * gain_vector


def contract(left, turned):
    return lax.dot_general(
        left, turned, (((1,), (1,)), ((), ())), preferred_element_type=jnp.float32
    )


def swap_blocks(x):
    return lax.all_to_all(x, "tp", 0, 0, tiled=True)


def summed_tokens(terms):
    tp_count = lax.axis_size("tp")
    tokens, width = terms.shape
    tiles = swap_blocks(terms.astype(jnp.bfloat16).reshape(tp_count, tokens // tp_count, width))
    return jnp.sum(tiles.astype(jnp.float32), axis=0).astype(jnp.bfloat16)


def shards(
    stream,
    in_gain,
    value_weight,
    gate_weight,
    conv_kernel,
    conv_gain,
    conv_shift,
    out_weight,
    norm_gain,
    up_weight,
    down_weight,
    out_gain,
):
    seq_count, seq_length, model_width = stream.shape
    token_count = seq_count * seq_length
    tp_count = lax.axis_size("tp")
    slice_width = model_width // tp_count
    own_tokens = token_count // tp_count
    tp_index = lax.axis_index("tp")
    channels = value_weight.shape[1]

    first = gather_fs(jnp.concatenate([value_weight, gate_weight, out_weight.T], axis=1))
    up_weight, first = lax.optimization_barrier((up_weight, first))
    up_whole = gather_fs(up_weight)
    down_weight, up_whole = lax.optimization_barrier((down_weight, up_whole))
    down_turned = gather_fs(down_weight.T)
    value_gate, out_turned = first[:, : 2 * channels], first[:, 2 * channels :]

    normed = norm_rows(
        stream.reshape(token_count, model_width).astype(jnp.float32), in_gain
    ).astype(jnp.bfloat16)
    both = jnp.dot(normed, value_gate, preferred_element_type=jnp.float32)
    gated = (both[:, :channels] * jax.nn.sigmoid(both[:, channels:])).astype(jnp.bfloat16)
    convolved = lax.conv_general_dilated(
        gated.reshape(seq_count, seq_length, channels),
        conv_kernel[:, None, :],
        window_strides=(1,),
        padding=[(KW - 1, 0)],
        dimension_numbers=("NWC", "WIO", "NWC"),
        feature_group_count=channels,
        preferred_element_type=jnp.float32,
    ).reshape(token_count, channels)
    sums = jnp.stack([jnp.sum(convolved, axis=1), jnp.sum(convolved * convolved, axis=1)])
    sums = jnp.sum(swap_blocks(jnp.broadcast_to(sums[None], (tp_count, *sums.shape))), axis=0)
    row_mean = sums[0] / (channels * tp_count)
    row_var = sums[1] / (channels * tp_count) - row_mean * row_mean
    activated = jax.nn.silu(
        (convolved - row_mean[:, None]) * lax.rsqrt(row_var + norm_epsilon)[:, None] * conv_gain
        + conv_shift
    ).astype(jnp.bfloat16)

    mixed = summed_tokens(contract(activated, out_turned))
    normed_own = lax.dynamic_slice_in_dim(normed, tp_index * own_tokens, own_tokens, 0)
    settled_own = norm_rows(
        residual_scale * normed_own.astype(jnp.float32) + mixed.astype(jnp.float32), norm_gain
    ).astype(jnp.bfloat16)
    settled = lax.all_gather(settled_own, "tp", axis=0, tiled=True)
    whole_gain = lax.all_gather(out_gain, "tp", axis=0, tiled=True)

    hidden = jnp.square(
        jax.nn.relu(jnp.dot(settled, up_whole, preferred_element_type=jnp.float32))
    ).astype(jnp.bfloat16)
    fed = summed_tokens(contract(hidden, down_turned))
    result_own = norm_rows(
        residual_scale * settled_own.astype(jnp.float32) + fed.astype(jnp.float32), whole_gain
    ).astype(jnp.bfloat16)
    pieces = jnp.moveaxis(result_own.reshape(own_tokens, tp_count, slice_width), 1, 0)
    result = swap_blocks(pieces)
    return result.reshape(seq_count, seq_length, slice_width)


def solution(mesh):
    in_specs = (
        P(("grp", "fs"), None, None),
        P(),
        P("fs", "tp"),
        P("fs", "tp"),
        P(None, "tp"),
        P("tp"),
        P("tp"),
        P("tp", "fs"),
        P(),
        P("fs", "tp"),
        P("tp", "fs"),
        P("tp"),
    )
    out_specs = P(("grp", "fs"), None, "tp")
    return jax.shard_map(shards, mesh=mesh, in_specs=in_specs, out_specs=out_specs, check_vma=False)
```

```python
import jax
import jax.numpy as jnp
from jax import lax
from jax.sharding import PartitionSpec as P

KW = 31

norm_epsilon = 1e-05
residual_scale = 2.0**0.25


def gather_fs(x):
    return lax.all_gather(x, "fs", axis=0, tiled=True)


def gather_in_pairs(even_part, odd_part):
    group_count = lax.axis_size("grp")
    if group_count % 2:
        return gather_fs(even_part), gather_fs(odd_part)
    is_even = lax.axis_index("grp") % 2 == 0
    mine = gather_fs(jnp.where(is_even, even_part, odd_part))
    theirs = lax.ppermute(mine, "grp", [(g, g ^ 1) for g in range(group_count)])
    return jnp.where(is_even, mine, theirs), jnp.where(is_even, theirs, mine)


def norm_rows(values, gain_vector):
    row_mean = jnp.mean(values, axis=-1, keepdims=True)
    row_var = jnp.mean(jnp.square(values - row_mean), axis=-1, keepdims=True)
    return (values - row_mean) * lax.rsqrt(row_var + norm_epsilon) * gain_vector


def contract(left, turned):
    return lax.dot_general(
        left, turned, (((1,), (1,)), ((), ())), preferred_element_type=jnp.float32
    )


def swap_blocks(x):
    return lax.all_to_all(x, "tp", 0, 0, tiled=True)


def summed_tokens(terms):
    tp_count = lax.axis_size("tp")
    tokens, width = terms.shape
    tiles = swap_blocks(terms.astype(jnp.bfloat16).reshape(tp_count, tokens // tp_count, width))
    return jnp.sum(tiles.astype(jnp.float32), axis=0).astype(jnp.bfloat16)


def shards(
    stream,
    in_gain,
    value_weight,
    gate_weight,
    conv_kernel,
    conv_gain,
    conv_shift,
    out_weight,
    norm_gain,
    up_weight,
    down_weight,
    out_gain,
):
    seq_count, seq_length, model_width = stream.shape
    token_count = seq_count * seq_length
    tp_count = lax.axis_size("tp")
    slice_width = model_width // tp_count
    own_tokens = token_count // tp_count
    tp_index = lax.axis_index("tp")
    channels = value_weight.shape[1]

    feed = gather_fs(jnp.concatenate([up_weight, down_weight.T], axis=1))
    hidden_count = up_weight.shape[1]
    up_whole, down_turned = feed[:, :hidden_count], feed[:, hidden_count:]

    rows = value_weight.shape[0]
    half = rows // 2
    out_shard = out_weight.T
    even_whole, odd_whole = gather_in_pairs(
        jnp.concatenate([value_weight, out_shard[:half]], axis=0),
        jnp.concatenate([gate_weight, out_shard[half:]], axis=0),
    )
    even_whole = even_whole.reshape(-1, rows + half, channels)
    odd_whole = odd_whole.reshape(-1, rows + half, channels)
    value_whole = even_whole[:, :rows].reshape(-1, channels)
    gate_whole = odd_whole[:, :rows].reshape(-1, channels)
    out_turned = jnp.concatenate([even_whole[:, rows:], odd_whole[:, rows:]], axis=1).reshape(-1, channels)

    normed = norm_rows(
        stream.reshape(token_count, model_width).astype(jnp.float32), in_gain
    ).astype(jnp.bfloat16)
    values = jnp.dot(normed, value_whole, preferred_element_type=jnp.float32)
    gating = jnp.dot(normed, gate_whole, preferred_element_type=jnp.float32)
    gated = (values * jax.nn.sigmoid(gating)).astype(jnp.bfloat16)
    convolved = lax.conv_general_dilated(
        gated.reshape(seq_count, seq_length, channels),
        conv_kernel[:, None, :],
        window_strides=(1,),
        padding=[(KW - 1, 0)],
        dimension_numbers=("NWC", "WIO", "NWC"),
        feature_group_count=channels,
        preferred_element_type=jnp.float32,
    ).reshape(token_count, channels)
    told = jnp.concatenate(
        [jnp.sum(convolved, axis=1), jnp.sum(convolved * convolved, axis=1), out_gain]
    )
    heard = swap_blocks(jnp.broadcast_to(told[None], (tp_count, *told.shape)))
    sums = jnp.sum(heard[:, : 2 * token_count], axis=0).reshape(2, token_count)
    whole_gain = heard[:, 2 * token_count :].reshape(model_width)
    row_mean = sums[0] / (channels * tp_count)
    row_var = sums[1] / (channels * tp_count) - row_mean * row_mean
    activated = jax.nn.silu(
        (convolved - row_mean[:, None]) * lax.rsqrt(row_var + norm_epsilon)[:, None] * conv_gain
        + conv_shift
    ).astype(jnp.bfloat16)

    mixed = summed_tokens(contract(activated, out_turned))
    normed_own = lax.dynamic_slice_in_dim(normed, tp_index * own_tokens, own_tokens, 0)
    settled_own = norm_rows(
        residual_scale * normed_own.astype(jnp.float32) + mixed.astype(jnp.float32), norm_gain
    ).astype(jnp.bfloat16)
    settled = lax.all_gather(settled_own, "tp", axis=0, tiled=True)

    hidden = jnp.square(
        jax.nn.relu(jnp.dot(settled, up_whole, preferred_element_type=jnp.float32))
    ).astype(jnp.bfloat16)
    fed = summed_tokens(contract(hidden, down_turned))
    result_own = norm_rows(
        residual_scale * settled_own.astype(jnp.float32) + fed.astype(jnp.float32), whole_gain
    ).astype(jnp.bfloat16)
    pieces = jnp.moveaxis(result_own.reshape(own_tokens, tp_count, slice_width), 1, 0)
    result = swap_blocks(pieces)
    return result.reshape(seq_count, seq_length, slice_width)


def solution(mesh):
    in_specs = (
        P(("grp", "fs"), None, None),
        P(),
        P("fs", "tp"),
        P("fs", "tp"),
        P(None, "tp"),
        P("tp"),
        P("tp"),
        P("tp", "fs"),
        P(),
        P("fs", "tp"),
        P("tp", "fs"),
        P("tp"),
    )
    out_specs = P(("grp", "fs"), None, "tp")
    return jax.shard_map(shards, mesh=mesh, in_specs=in_specs, out_specs=out_specs, check_vma=False)
```

```python
import jax
import jax.numpy as jnp
from jax import lax
from jax.sharding import PartitionSpec as P


KW = 31

norm_epsilon = 1e-05
residual_scale = 2.0**0.25
half_scale = 2.0**18


def gather_fs(x):
    return lax.all_gather(x, "fs", axis=0, tiled=True)


def to_half(x):
    return (x.astype(jnp.float32) * half_scale).astype(jnp.float16)


def from_half(x):
    return (x.astype(jnp.float32) * (1 / half_scale)).astype(jnp.bfloat16)


def norm_rows(values, gain_vector):
    row_mean = jnp.mean(values, axis=-1, keepdims=True)
    row_var = jnp.mean(jnp.square(values - row_mean), axis=-1, keepdims=True)
    return (values - row_mean) * lax.rsqrt(row_var + norm_epsilon) * gain_vector


def contract(left, turned):
    return lax.dot_general(
        left, turned, (((1,), (1,)), ((), ())), preferred_element_type=jnp.float32
    )


def swap_blocks(x):
    return lax.all_to_all(x, "tp", 0, 0, tiled=True)


def summed_tokens(terms):
    tp_count = lax.axis_size("tp")
    tokens, width = terms.shape
    tiles = swap_blocks(terms.astype(jnp.bfloat16).reshape(tp_count, tokens // tp_count, width))
    return jnp.sum(tiles.astype(jnp.float32), axis=0).astype(jnp.bfloat16)


def shards(
    stream,
    in_gain,
    value_weight,
    gate_weight,
    conv_kernel,
    conv_gain,
    conv_shift,
    out_weight,
    norm_gain,
    up_weight,
    down_weight,
    out_gain,
):
    seq_count, seq_length, model_width = stream.shape
    token_count = seq_count * seq_length
    tp_count = lax.axis_size("tp")
    slice_width = model_width // tp_count
    own_tokens = token_count // tp_count
    tp_index = lax.axis_index("tp")
    channels = value_weight.shape[1]

    down_turned = gather_fs(down_weight.T)

    group_count = lax.axis_size("grp")
    paired = group_count % 2 == 0
    is_even = lax.axis_index("grp") % 2 == 0
    hidden_half = up_weight.shape[1] // 2
    low_up, high_up = up_weight[:, :hidden_half], up_weight[:, hidden_half:]
    own_up = jnp.where(is_even, low_up, high_up) if paired else up_weight
    early = gather_fs(
        to_half(jnp.concatenate([value_weight, gate_weight, out_weight.T, own_up], axis=1))
    )
    value_whole = from_half(early[:, :channels])
    gate_whole = from_half(early[:, channels : 2 * channels])
    out_turned = from_half(early[:, 2 * channels : 3 * channels])
    up_parts = [early[:, 3 * channels :]]
    if paired:
        up_parts.append(lax.ppermute(up_parts[0], "grp", [(g, g ^ 1) for g in range(group_count)]))

    normed = norm_rows(
        stream.reshape(token_count, model_width).astype(jnp.float32), in_gain
    ).astype(jnp.bfloat16)
    values = jnp.dot(normed, value_whole, preferred_element_type=jnp.float32)
    gating = jnp.dot(normed, gate_whole, preferred_element_type=jnp.float32)
    gated = (values * jax.nn.sigmoid(gating)).astype(jnp.bfloat16)
    convolved = lax.conv_general_dilated(
        gated.reshape(seq_count, seq_length, channels),
        conv_kernel[:, None, :],
        window_strides=(1,),
        padding=[(KW - 1, 0)],
        dimension_numbers=("NWC", "WIO", "NWC"),
        feature_group_count=channels,
        preferred_element_type=jnp.float32,
    ).reshape(token_count, channels)
    told = jnp.concatenate(
        [jnp.sum(convolved, axis=1), jnp.sum(convolved * convolved, axis=1), out_gain]
    )
    heard = swap_blocks(jnp.broadcast_to(told[None], (tp_count, *told.shape)))
    sums = jnp.sum(heard[:, : 2 * token_count], axis=0).reshape(2, token_count)
    whole_gain = heard[:, 2 * token_count :].reshape(model_width)
    row_mean = sums[0] / (channels * tp_count)
    row_var = sums[1] / (channels * tp_count) - row_mean * row_mean
    activated = jax.nn.silu(
        (convolved - row_mean[:, None]) * lax.rsqrt(row_var + norm_epsilon)[:, None] * conv_gain
        + conv_shift
    ).astype(jnp.bfloat16)

    mixed = summed_tokens(contract(activated, out_turned))
    normed_own = lax.dynamic_slice_in_dim(normed, tp_index * own_tokens, own_tokens, 0)
    settled_own = norm_rows(
        residual_scale * normed_own.astype(jnp.float32) + mixed.astype(jnp.float32), norm_gain
    ).astype(jnp.bfloat16)
    settled = lax.all_gather(settled_own, "tp", axis=0, tiled=True)

    hidden_parts = [
        jnp.square(
            jax.nn.relu(jnp.dot(settled, from_half(part), preferred_element_type=jnp.float32))
        ).astype(jnp.bfloat16)
        for part in up_parts
    ]
    if paired:
        mine, theirs = hidden_parts
        hidden_parts = [jnp.where(is_even, mine, theirs), jnp.where(is_even, theirs, mine)]
    hidden = lax.optimization_barrier(jnp.concatenate(hidden_parts, axis=1))
    fed = summed_tokens(contract(hidden, down_turned))
    result_own = norm_rows(
        residual_scale * settled_own.astype(jnp.float32) + fed.astype(jnp.float32), whole_gain
    ).astype(jnp.bfloat16)
    pieces = jnp.moveaxis(result_own.reshape(own_tokens, tp_count, slice_width), 1, 0)
    result = swap_blocks(pieces)
    return result.reshape(seq_count, seq_length, slice_width)


def solution(mesh):
    in_specs = (
        P(("grp", "fs"), None, None),
        P(),
        P("fs", "tp"),
        P("fs", "tp"),
        P(None, "tp"),
        P("tp"),
        P("tp"),
        P("tp", "fs"),
        P(),
        P("fs", "tp"),
        P("tp", "fs"),
        P("tp"),
    )
    out_specs = P(("grp", "fs"), None, "tp")
    return jax.shard_map(shards, mesh=mesh, in_specs=in_specs, out_specs=out_specs, check_vma=False)
```

```python
import jax
import jax.numpy as jnp
from jax import lax
from jax.sharding import PartitionSpec as P

KW = 31

norm_epsilon = 1e-05
residual_scale = 2.0**0.25
weight_scale = 2.0**18
feature_scale = 2.0**7


def to_half(x, scale):
    return (x.astype(jnp.float32) * scale).astype(jnp.float16)


def from_half(x, scale):
    return (x.astype(jnp.float32) * (1 / scale)).astype(jnp.bfloat16)


def norm_rows(values, gain_vector):
    row_mean = jnp.mean(values, axis=-1, keepdims=True)
    row_var = jnp.mean(jnp.square(values - row_mean), axis=-1, keepdims=True)
    return (values - row_mean) * lax.rsqrt(row_var + norm_epsilon) * gain_vector


def contract(left, turned):
    return lax.dot_general(
        left, turned, (((1,), (1,)), ((), ())), preferred_element_type=jnp.float32
    )


def swap_blocks(x):
    return lax.all_to_all(x, "tp", 0, 0, tiled=True)


def summed(tiles):
    return jnp.sum(tiles.astype(jnp.float32), axis=0).astype(jnp.bfloat16)


def shards(
    stream,
    in_gain,
    value_weight,
    gate_weight,
    conv_kernel,
    conv_gain,
    conv_shift,
    out_weight,
    norm_gain,
    up_weight,
    down_weight,
    out_gain,
):
    seq_count, seq_length, model_width = stream.shape
    token_count = seq_count * seq_length
    tp_count = lax.axis_size("tp")
    group_count = lax.axis_size("grp")
    slice_width = model_width // tp_count
    own_tokens = token_count // tp_count
    tp_index = lax.axis_index("tp")
    channels = value_weight.shape[1]

    sharing = 2 if group_count % 2 == 0 else 1
    teams = [
        [g * tp_count + t for g in range(first, first + sharing) for t in range(tp_count)]
        for first in range(0, group_count, sharing)
    ]
    share = up_weight.shape[1] // sharing
    up_shard, down_shard = up_weight, down_weight.T
    if sharing == 2:
        is_even = lax.axis_index("grp") % 2 == 0
        up_shard = jnp.where(is_even, up_shard[:, :share], up_shard[:, share:])
        down_shard = jnp.where(is_even, down_shard[:, :share], down_shard[:, share:])
    whole = lax.all_gather(
        to_half(
            jnp.concatenate(
                [
                    value_weight,
                    gate_weight,
                    out_weight.T,
                    lax.optimization_barrier(jnp.concatenate([up_shard, down_shard], axis=1)),
                ],
                axis=1,
            ),
            weight_scale,
        ),
        "fs",
        axis=0,
        tiled=True,
    )
    ends = [channels, 2 * channels, 3 * channels, 3 * channels + share]
    value_whole, gate_whole, out_turned, up_whole, down_turned = (
        from_half(part, weight_scale) for part in jnp.split(whole, ends, axis=1)
    )

    normed = norm_rows(
        stream.reshape(token_count, model_width).astype(jnp.float32), in_gain
    ).astype(jnp.bfloat16)
    values = jnp.dot(normed, value_whole, preferred_element_type=jnp.float32)
    gating = jnp.dot(normed, gate_whole, preferred_element_type=jnp.float32)
    gated = (values * jax.nn.sigmoid(gating)).astype(jnp.bfloat16)
    convolved = lax.conv_general_dilated(
        gated.reshape(seq_count, seq_length, channels),
        conv_kernel[:, None, :],
        window_strides=(1,),
        padding=[(KW - 1, 0)],
        dimension_numbers=("NWC", "WIO", "NWC"),
        feature_group_count=channels,
        preferred_element_type=jnp.float32,
    ).reshape(token_count, channels)
    told = jnp.concatenate(
        [jnp.sum(convolved, axis=1), jnp.sum(convolved * convolved, axis=1), out_gain]
    )
    heard = swap_blocks(jnp.broadcast_to(told[None], (tp_count, *told.shape)))
    sums = jnp.sum(heard[:, : 2 * token_count], axis=0).reshape(2, token_count)
    whole_gain = heard[:, 2 * token_count :].reshape(model_width)
    row_mean = sums[0] / (channels * tp_count)
    row_var = sums[1] / (channels * tp_count) - row_mean * row_mean
    activated = jax.nn.silu(
        (convolved - row_mean[:, None]) * lax.rsqrt(row_var + norm_epsilon)[:, None] * conv_gain
        + conv_shift
    ).astype(jnp.bfloat16)

    mixed_terms = contract(activated, out_turned).astype(jnp.bfloat16)
    mixed = summed(swap_blocks(mixed_terms.reshape(tp_count, own_tokens, model_width)))
    normed_own = lax.dynamic_slice_in_dim(normed, tp_index * own_tokens, own_tokens, 0)
    settled_own = norm_rows(
        residual_scale * normed_own.astype(jnp.float32) + mixed.astype(jnp.float32), norm_gain
    ).astype(jnp.bfloat16)
    settled = from_half(
        lax.all_gather(
            to_half(settled_own, feature_scale),
            ("grp", "tp"),
            axis=0,
            tiled=True,
            axis_index_groups=teams,
        ),
        feature_scale,
    )

    hidden = jnp.square(
        jax.nn.relu(jnp.dot(settled, up_whole, preferred_element_type=jnp.float32))
    ).astype(jnp.bfloat16)
    hidden = lax.optimization_barrier(hidden)
    fed_terms = contract(hidden, down_turned).astype(jnp.bfloat16)
    fed = summed(
        lax.all_to_all(
            fed_terms.reshape(sharing * tp_count, own_tokens, model_width),
            ("grp", "tp"),
            0,
            0,
            tiled=True,
            axis_index_groups=teams,
        )
    )
    result_own = norm_rows(
        residual_scale * settled_own.astype(jnp.float32) + fed.astype(jnp.float32), whole_gain
    ).astype(jnp.bfloat16)
    pieces = jnp.moveaxis(result_own.reshape(own_tokens, tp_count, slice_width), 1, 0)
    return swap_blocks(pieces).reshape(seq_count, seq_length, slice_width)


def solution(mesh):
    in_specs = (
        P(("grp", "fs"), None, None),
        P(),
        P("fs", "tp"),
        P("fs", "tp"),
        P(None, "tp"),
        P("tp"),
        P("tp"),
        P("tp", "fs"),
        P(),
        P("fs", "tp"),
        P("tp", "fs"),
        P("tp"),
    )
    out_specs = P(("grp", "fs"), None, "tp")
    return jax.shard_map(shards, mesh=mesh, in_specs=in_specs, out_specs=out_specs, check_vma=False)
```

```python
import jax
import jax.numpy as jnp
from jax import lax
from jax.sharding import PartitionSpec as P

KW = 31

norm_epsilon = 1e-05
residual_scale = 2.0**0.25
feature_scale = 2.0**7


def to_half(x, scale):
    return (x.astype(jnp.float32) * scale).astype(jnp.float16)


def from_half(x, scale):
    return (x.astype(jnp.float32) * (1 / scale)).astype(jnp.bfloat16)


def gather_fs(x):
    return lax.all_gather(x, "fs", axis=0, tiled=True)


def in_order(is_even, mine, theirs):
    return jnp.where(is_even, mine, theirs), jnp.where(is_even, theirs, mine)


def norm_rows(values, gain_vector):
    row_mean = jnp.mean(values, axis=-1, keepdims=True)
    row_var = jnp.mean(jnp.square(values - row_mean), axis=-1, keepdims=True)
    return (values - row_mean) * lax.rsqrt(row_var + norm_epsilon) * gain_vector


def contract(left, turned):
    return lax.dot_general(
        left, turned, (((1,), (1,)), ((), ())), preferred_element_type=jnp.float32
    )


def swap_blocks(x):
    return lax.all_to_all(x, "tp", 0, 0, tiled=True)


def summed(tiles):
    return jnp.sum(tiles.astype(jnp.float32), axis=0).astype(jnp.bfloat16)


def shards(
    stream,
    in_gain,
    value_weight,
    gate_weight,
    conv_kernel,
    conv_gain,
    conv_shift,
    out_weight,
    norm_gain,
    up_weight,
    down_weight,
    out_gain,
):
    seq_count, seq_length, model_width = stream.shape
    token_count = seq_count * seq_length
    tp_count = lax.axis_size("tp")
    group_count = lax.axis_size("grp")
    slice_width = model_width // tp_count
    own_tokens = token_count // tp_count
    tp_index = lax.axis_index("tp")
    channels = value_weight.shape[1]

    sharing = 2 if group_count % 2 == 0 else 1
    partner = [(g, g ^ 1) for g in range(group_count)]
    is_even = lax.axis_index("grp") % 2 == 0
    teams = [
        [g * tp_count + t for g in range(first, first + sharing) for t in range(tp_count)]
        for first in range(0, group_count, sharing)
    ]
    share = up_weight.shape[1] // sharing
    up_shard, down_shard = up_weight, down_weight.T
    if sharing == 2:
        up_shard = jnp.where(is_even, up_shard[:, :share], up_shard[:, share:])
        down_shard = jnp.where(is_even, down_shard[:, :share], down_shard[:, share:])
    feed = gather_fs(jnp.concatenate([up_shard, down_shard], axis=1))
    up_whole, down_turned = feed[:, :share], feed[:, share:]

    rows = value_weight.shape[0]
    half = rows // 2
    out_shard = out_weight.T
    even_part = jnp.concatenate([value_weight, out_shard[:half]], axis=0)
    odd_part = jnp.concatenate([gate_weight, out_shard[half:]], axis=0)
    if sharing == 2:
        mine = gather_fs(jnp.where(is_even, even_part, odd_part))
        theirs = lax.ppermute(mine, "grp", partner)
        even_whole, odd_whole = in_order(is_even, mine, theirs)
    else:
        even_whole, odd_whole = gather_fs(even_part), gather_fs(odd_part)
    even_whole = even_whole.reshape(-1, rows + half, channels)
    odd_whole = odd_whole.reshape(-1, rows + half, channels)
    value_whole = even_whole[:, :rows].reshape(-1, channels)
    gate_whole = odd_whole[:, :rows].reshape(-1, channels)
    out_turned = jnp.concatenate([even_whole[:, rows:], odd_whole[:, rows:]], axis=1).reshape(-1, channels)

    normed = norm_rows(
        stream.reshape(token_count, model_width).astype(jnp.float32), in_gain
    ).astype(jnp.bfloat16)
    values = jnp.dot(normed, value_whole, preferred_element_type=jnp.float32)
    gating = jnp.dot(normed, gate_whole, preferred_element_type=jnp.float32)
    gated = (values * jax.nn.sigmoid(gating)).astype(jnp.bfloat16)
    convolved = lax.conv_general_dilated(
        gated.reshape(seq_count, seq_length, channels),
        conv_kernel[:, None, :],
        window_strides=(1,),
        padding=[(KW - 1, 0)],
        dimension_numbers=("NWC", "WIO", "NWC"),
        feature_group_count=channels,
        preferred_element_type=jnp.float32,
    ).reshape(token_count, channels)
    told = jnp.concatenate(
        [jnp.sum(convolved, axis=1), jnp.sum(convolved * convolved, axis=1), out_gain]
    )
    heard = swap_blocks(jnp.broadcast_to(told[None], (tp_count, *told.shape)))
    sums = jnp.sum(heard[:, : 2 * token_count], axis=0).reshape(2, token_count)
    whole_gain = heard[:, 2 * token_count :].reshape(model_width)
    row_mean = sums[0] / (channels * tp_count)
    row_var = sums[1] / (channels * tp_count) - row_mean * row_mean
    activated = jax.nn.silu(
        (convolved - row_mean[:, None]) * lax.rsqrt(row_var + norm_epsilon)[:, None] * conv_gain
        + conv_shift
    ).astype(jnp.bfloat16)

    mixed_terms = contract(activated, out_turned).astype(jnp.bfloat16)
    mixed = summed(swap_blocks(mixed_terms.reshape(tp_count, own_tokens, model_width)))
    normed_own = lax.dynamic_slice_in_dim(normed, tp_index * own_tokens, own_tokens, 0)
    settled_own = norm_rows(
        residual_scale * normed_own.astype(jnp.float32) + mixed.astype(jnp.float32), norm_gain
    ).astype(jnp.bfloat16)
    if sharing == 2:
        their_settled = lax.ppermute(settled_own, "grp", partner)
        pair_settled = jnp.stack(in_order(is_even, settled_own, their_settled))
    else:
        pair_settled = settled_own[None]
    settled = from_half(
        lax.all_gather(to_half(pair_settled, feature_scale), "tp", axis=1, tiled=True),
        feature_scale,
    ).reshape(sharing * token_count, model_width)

    hidden = jnp.square(
        jax.nn.relu(jnp.dot(settled, up_whole, preferred_element_type=jnp.float32))
    ).astype(jnp.bfloat16)
    hidden = lax.optimization_barrier(hidden)
    fed_terms = contract(hidden, down_turned).astype(jnp.bfloat16)
    fed = summed(
        lax.all_to_all(
            fed_terms.reshape(sharing * tp_count, own_tokens, model_width),
            ("grp", "tp"),
            0,
            0,
            tiled=True,
            axis_index_groups=teams,
        )
    )
    result_own = norm_rows(
        residual_scale * settled_own.astype(jnp.float32) + fed.astype(jnp.float32), whole_gain
    ).astype(jnp.bfloat16)
    pieces = jnp.moveaxis(result_own.reshape(own_tokens, tp_count, slice_width), 1, 0)
    return swap_blocks(pieces).reshape(seq_count, seq_length, slice_width)


def solution(mesh):
    in_specs = (
        P(("grp", "fs"), None, None),
        P(),
        P("fs", "tp"),
        P("fs", "tp"),
        P(None, "tp"),
        P("tp"),
        P("tp"),
        P("tp", "fs"),
        P(),
        P("fs", "tp"),
        P("tp", "fs"),
        P("tp"),
    )
    out_specs = P(("grp", "fs"), None, "tp")
    return jax.shard_map(shards, mesh=mesh, in_specs=in_specs, out_specs=out_specs, check_vma=False)
```

```python
import jax
import jax.numpy as jnp
from jax import lax
from jax.sharding import PartitionSpec as P

KW = 31

norm_epsilon = 1e-05
residual_scale = 2.0**0.25
feature_scale = 2.0**7


def to_half(x, scale):
    return (x.astype(jnp.float32) * scale).astype(jnp.float16)


def from_half(x, scale):
    return (x.astype(jnp.float32) * (1 / scale)).astype(jnp.bfloat16)


def gather_fs(x):
    return lax.all_gather(x, "fs", axis=0, tiled=True)


def in_order(is_even, mine, theirs):
    return jnp.where(is_even, mine, theirs), jnp.where(is_even, theirs, mine)


def norm_rows(values, gain_vector):
    row_mean = jnp.mean(values, axis=-1, keepdims=True)
    row_var = jnp.mean(jnp.square(values - row_mean), axis=-1, keepdims=True)
    return (values - row_mean) * lax.rsqrt(row_var + norm_epsilon) * gain_vector


def contract(left, turned):
    return lax.dot_general(
        left, turned, (((1,), (1,)), ((), ())), preferred_element_type=jnp.float32
    )


def swap_blocks(x):
    return lax.all_to_all(x, "tp", 0, 0, tiled=True)


def summed(tiles):
    return jnp.sum(tiles.astype(jnp.float32), axis=0).astype(jnp.bfloat16)


def shards(
    stream,
    in_gain,
    value_weight,
    gate_weight,
    conv_kernel,
    conv_gain,
    conv_shift,
    out_weight,
    norm_gain,
    up_weight,
    down_weight,
    out_gain,
):
    seq_count, seq_length, model_width = stream.shape
    token_count = seq_count * seq_length
    tp_count = lax.axis_size("tp")
    group_count = lax.axis_size("grp")
    slice_width = model_width // tp_count
    own_tokens = token_count // tp_count
    tp_index = lax.axis_index("tp")
    channels = value_weight.shape[1]

    sharing = 2 if group_count % 2 == 0 else 1
    partner = [(g, g ^ 1) for g in range(group_count)]
    is_even = lax.axis_index("grp") % 2 == 0
    teams = [
        [g * tp_count + t for g in range(first, first + sharing) for t in range(tp_count)]
        for first in range(0, group_count, sharing)
    ]
    share = up_weight.shape[1] // sharing
    up_shard, down_shard = up_weight, down_weight.T
    if sharing == 2:
        up_shard = jnp.where(is_even, up_shard[:, :share], up_shard[:, share:])
        down_shard = jnp.where(is_even, down_shard[:, :share], down_shard[:, share:])
    feed = gather_fs(jnp.concatenate([up_shard, down_shard], axis=1))
    up_whole, down_turned = feed[:, :share], feed[:, share:]

    rows = value_weight.shape[0]
    half = rows // 2
    out_shard = out_weight.T
    even_part = jnp.concatenate([value_weight, out_shard[:half]], axis=0)
    odd_part = jnp.concatenate([gate_weight, out_shard[half:]], axis=0)
    if sharing == 2:
        mine = gather_fs(jnp.where(is_even, even_part, odd_part))
        theirs = lax.ppermute(mine, "grp", partner)
        even_whole, odd_whole = in_order(is_even, mine, theirs)
    else:
        even_whole, odd_whole = gather_fs(even_part), gather_fs(odd_part)
    even_whole = even_whole.reshape(-1, rows + half, channels)
    odd_whole = odd_whole.reshape(-1, rows + half, channels)
    value_whole = even_whole[:, :rows].reshape(-1, channels)
    gate_whole = odd_whole[:, :rows].reshape(-1, channels)
    out_turned = jnp.concatenate([even_whole[:, rows:], odd_whole[:, rows:]], axis=1).reshape(-1, channels)

    normed = norm_rows(
        stream.reshape(token_count, model_width).astype(jnp.float32), in_gain
    ).astype(jnp.bfloat16)
    values = jnp.dot(normed, value_whole, preferred_element_type=jnp.float32)
    gating = jnp.dot(normed, gate_whole, preferred_element_type=jnp.float32)
    gated = (values * jax.nn.sigmoid(gating)).astype(jnp.bfloat16)
    convolved = lax.conv_general_dilated(
        gated.reshape(seq_count, seq_length, channels),
        conv_kernel[:, None, :],
        window_strides=(1,),
        padding=[(KW - 1, 0)],
        dimension_numbers=("NWC", "WIO", "NWC"),
        feature_group_count=channels,
        preferred_element_type=jnp.float32,
    ).reshape(token_count, channels)
    told = jnp.concatenate(
        [jnp.sum(convolved, axis=1), jnp.sum(convolved * convolved, axis=1), out_gain]
    )
    normed_own = lax.dynamic_slice_in_dim(normed, tp_index * own_tokens, own_tokens, 0)
    told, out_turned, normed_own, norm_gain = lax.optimization_barrier(
        (told, out_turned, normed_own, norm_gain)
    )
    heard = swap_blocks(jnp.broadcast_to(told[None], (tp_count, *told.shape)))
    sums = jnp.sum(heard[:, : 2 * token_count], axis=0).reshape(2, token_count)
    whole_gain = heard[:, 2 * token_count :].reshape(model_width)
    row_mean = sums[0] / (channels * tp_count)
    row_var = sums[1] / (channels * tp_count) - row_mean * row_mean
    activated = jax.nn.silu(
        (convolved - row_mean[:, None]) * lax.rsqrt(row_var + norm_epsilon)[:, None] * conv_gain
        + conv_shift
    ).astype(jnp.bfloat16)

    mixed_terms = contract(activated, out_turned).astype(jnp.bfloat16)
    mixed_terms, whole_gain = lax.optimization_barrier((mixed_terms, whole_gain))
    mixed = summed(swap_blocks(mixed_terms.reshape(tp_count, own_tokens, model_width)))
    settled_own = norm_rows(
        residual_scale * normed_own.astype(jnp.float32) + mixed.astype(jnp.float32), norm_gain
    ).astype(jnp.bfloat16)
    if sharing == 2:
        their_settled = lax.ppermute(settled_own, "grp", partner)
        pair_settled = jnp.stack(in_order(is_even, settled_own, their_settled))
    else:
        pair_settled = settled_own[None]
    settled = from_half(
        lax.all_gather(to_half(pair_settled, feature_scale), "tp", axis=1, tiled=True),
        feature_scale,
    ).reshape(sharing * token_count, model_width)

    hidden = jnp.square(
        jax.nn.relu(jnp.dot(settled, up_whole, preferred_element_type=jnp.float32))
    ).astype(jnp.bfloat16)
    hidden = lax.optimization_barrier(hidden)
    fed_terms = contract(hidden, down_turned).astype(jnp.bfloat16)
    fed = summed(
        lax.all_to_all(
            fed_terms.reshape(sharing * tp_count, own_tokens, model_width),
            ("grp", "tp"),
            0,
            0,
            tiled=True,
            axis_index_groups=teams,
        )
    )
    result_own = norm_rows(
        residual_scale * settled_own.astype(jnp.float32) + fed.astype(jnp.float32), whole_gain
    ).astype(jnp.bfloat16)
    pieces = jnp.moveaxis(result_own.reshape(own_tokens, tp_count, slice_width), 1, 0)
    return swap_blocks(pieces).reshape(seq_count, seq_length, slice_width)


def solution(mesh):
    in_specs = (
        P(("grp", "fs"), None, None),
        P(),
        P("fs", "tp"),
        P("fs", "tp"),
        P(None, "tp"),
        P("tp"),
        P("tp"),
        P("tp", "fs"),
        P(),
        P("fs", "tp"),
        P("tp", "fs"),
        P("tp"),
    )
    out_specs = P(("grp", "fs"), None, "tp")
    return jax.shard_map(shards, mesh=mesh, in_specs=in_specs, out_specs=out_specs, check_vma=False)
```

```python
import jax
import jax.numpy as jnp
from jax import lax
from jax.sharding import PartitionSpec as P

KW = 31

norm_epsilon = 1e-05
residual_scale = 2.0**0.25
feature_scale = 2.0**7


def to_half(x, scale):
    return (x.astype(jnp.float32) * scale).astype(jnp.float16)


def from_half(x, scale):
    return (x.astype(jnp.float32) * (1 / scale)).astype(jnp.bfloat16)


def gather_fs(x):
    return lax.all_gather(x, "fs", axis=0, tiled=True)


def in_order(is_even, mine, theirs):
    return jnp.where(is_even, mine, theirs), jnp.where(is_even, theirs, mine)


def norm_rows(values, gain_vector):
    row_mean = jnp.mean(values, axis=-1, keepdims=True)
    row_var = jnp.mean(jnp.square(values - row_mean), axis=-1, keepdims=True)
    return (values - row_mean) * lax.rsqrt(row_var + norm_epsilon) * gain_vector


def contract(left, turned):
    return lax.dot_general(
        left, turned, (((1,), (1,)), ((), ())), preferred_element_type=jnp.float32
    )


def swap_blocks(x):
    return lax.all_to_all(x, "tp", 0, 0, tiled=True)


def summed(tiles):
    return jnp.sum(tiles.astype(jnp.float32), axis=0).astype(jnp.bfloat16)


def shards(
    stream,
    in_gain,
    value_weight,
    gate_weight,
    conv_kernel,
    conv_gain,
    conv_shift,
    out_weight,
    norm_gain,
    up_weight,
    down_weight,
    out_gain,
):
    seq_count, seq_length, model_width = stream.shape
    token_count = seq_count * seq_length
    tp_count = lax.axis_size("tp")
    group_count = lax.axis_size("grp")
    slice_width = model_width // tp_count
    own_tokens = token_count // tp_count
    tp_index = lax.axis_index("tp")
    channels = value_weight.shape[1]

    sharing = 2 if group_count % 2 == 0 else 1
    partner = [(g, g ^ 1) for g in range(group_count)]
    is_even = lax.axis_index("grp") % 2 == 0
    teams = [
        [g * tp_count + t for t in range(tp_count) for g in range(first, first + sharing)]
        for first in range(0, group_count, sharing)
    ]
    share = up_weight.shape[1] // sharing
    up_shard, down_shard = up_weight, down_weight.T
    if sharing == 2:
        up_shard = jnp.where(is_even, up_shard[:, :share], up_shard[:, share:])
        down_shard = jnp.where(is_even, down_shard[:, :share], down_shard[:, share:])
    feed = gather_fs(jnp.concatenate([up_shard, down_shard], axis=1))
    up_whole, down_turned = feed[:, :share], feed[:, share:]

    rows = value_weight.shape[0]
    half = rows // 2
    out_shard = out_weight.T
    even_part = jnp.concatenate([value_weight, out_shard[:half]], axis=0)
    odd_part = jnp.concatenate([gate_weight, out_shard[half:]], axis=0)
    if sharing == 2:
        mine = gather_fs(jnp.where(is_even, even_part, odd_part))
        theirs = lax.ppermute(mine, "grp", partner)
        even_whole, odd_whole = in_order(is_even, mine, theirs)
    else:
        even_whole, odd_whole = gather_fs(even_part), gather_fs(odd_part)
    even_whole = even_whole.reshape(-1, rows + half, channels)
    odd_whole = odd_whole.reshape(-1, rows + half, channels)
    value_whole = even_whole[:, :rows].reshape(-1, channels)
    gate_whole = odd_whole[:, :rows].reshape(-1, channels)
    out_turned = jnp.concatenate([even_whole[:, rows:], odd_whole[:, rows:]], axis=1).reshape(-1, channels)

    normed = norm_rows(
        stream.reshape(token_count, model_width).astype(jnp.float32), in_gain
    ).astype(jnp.bfloat16)
    values = jnp.dot(normed, value_whole, preferred_element_type=jnp.float32)
    gating = jnp.dot(normed, gate_whole, preferred_element_type=jnp.float32)
    gated = (values * jax.nn.sigmoid(gating)).astype(jnp.bfloat16)
    convolved = lax.conv_general_dilated(
        gated.reshape(seq_count, seq_length, channels),
        conv_kernel[:, None, :],
        window_strides=(1,),
        padding=[(KW - 1, 0)],
        dimension_numbers=("NWC", "WIO", "NWC"),
        feature_group_count=channels,
        preferred_element_type=jnp.float32,
    ).reshape(token_count, channels)
    told = jnp.concatenate(
        [jnp.sum(convolved, axis=1), jnp.sum(convolved * convolved, axis=1), out_gain]
    )
    normed_own = lax.dynamic_slice_in_dim(normed, tp_index * own_tokens, own_tokens, 0)
    told, out_turned, normed_own, norm_gain = lax.optimization_barrier(
        (told, out_turned, normed_own, norm_gain)
    )
    heard = swap_blocks(jnp.broadcast_to(told[None], (tp_count, *told.shape)))
    sums = jnp.sum(heard[:, : 2 * token_count], axis=0).reshape(2, token_count)
    whole_gain = heard[:, 2 * token_count :].reshape(model_width)
    row_mean = sums[0] / (channels * tp_count)
    row_var = sums[1] / (channels * tp_count) - row_mean * row_mean
    activated = jax.nn.silu(
        (convolved - row_mean[:, None]) * lax.rsqrt(row_var + norm_epsilon)[:, None] * conv_gain
        + conv_shift
    ).astype(jnp.bfloat16)

    mixed_terms = contract(activated, out_turned).astype(jnp.bfloat16)
    mixed_terms, whole_gain = lax.optimization_barrier((mixed_terms, whole_gain))
    mixed = summed(swap_blocks(mixed_terms.reshape(tp_count, own_tokens, model_width)))
    settled_own = norm_rows(
        residual_scale * normed_own.astype(jnp.float32) + mixed.astype(jnp.float32), norm_gain
    ).astype(jnp.bfloat16)
    if sharing == 2:
        their_settled = lax.ppermute(settled_own, "grp", partner)
        pair_settled = jnp.stack(in_order(is_even, settled_own, their_settled))
    else:
        pair_settled = settled_own[None]
    settled = from_half(
        lax.all_gather(to_half(pair_settled, feature_scale), "tp", axis=0, tiled=True),
        feature_scale,
    ).reshape(sharing * token_count, model_width)

    hidden = jnp.square(
        jax.nn.relu(jnp.dot(settled, up_whole, preferred_element_type=jnp.float32))
    ).astype(jnp.bfloat16)
    hidden = lax.optimization_barrier(hidden)
    fed_terms = contract(hidden, down_turned).astype(jnp.bfloat16)
    fed = summed(
        lax.all_to_all(
            fed_terms.reshape(sharing * tp_count, own_tokens, model_width),
            ("grp", "tp"),
            0,
            0,
            tiled=True,
            axis_index_groups=teams,
        )
    )
    result_own = norm_rows(
        residual_scale * settled_own.astype(jnp.float32) + fed.astype(jnp.float32), whole_gain
    ).astype(jnp.bfloat16)
    pieces = jnp.moveaxis(result_own.reshape(own_tokens, tp_count, slice_width), 1, 0)
    return swap_blocks(pieces).reshape(seq_count, seq_length, slice_width)


def solution(mesh):
    in_specs = (
        P(("grp", "fs"), None, None),
        P(),
        P("fs", "tp"),
        P("fs", "tp"),
        P(None, "tp"),
        P("tp"),
        P("tp"),
        P("tp", "fs"),
        P(),
        P("fs", "tp"),
        P("tp", "fs"),
        P("tp"),
    )
    out_specs = P(("grp", "fs"), None, "tp")
    return jax.shard_map(shards, mesh=mesh, in_specs=in_specs, out_specs=out_specs, check_vma=False)
```

```python
import jax
import jax.numpy as jnp
from jax import lax
from jax.sharding import PartitionSpec as P

KW = 31

norm_epsilon = 1e-05
residual_scale = 2.0**0.25
feature_scale = 2.0**7


def to_half(x, scale):
    return (x.astype(jnp.float32) * scale).astype(jnp.float16)


def from_half(x, scale):
    return (x.astype(jnp.float32) * (1 / scale)).astype(jnp.bfloat16)


def gather_fs(x):
    return lax.all_gather(x, "fs", axis=0, tiled=True)


def gather_in_strides(x):
    count = lax.axis_size("fs")
    if count % 2:
        return gather_fs(x)
    pairs = [[i, i + 1] for i in range(0, count, 2)]
    strides = [list(range(first, count, 2)) for first in range(2)]
    both = lax.all_gather(x, "fs", axis=0, tiled=True, axis_index_groups=pairs)
    return lax.all_gather(both, "fs", axis=0, tiled=True, axis_index_groups=strides)


def in_order(is_even, mine, theirs):
    return jnp.where(is_even, mine, theirs), jnp.where(is_even, theirs, mine)


def norm_rows(values, gain_vector):
    row_mean = jnp.mean(values, axis=-1, keepdims=True)
    row_var = jnp.mean(jnp.square(values - row_mean), axis=-1, keepdims=True)
    return (values - row_mean) * lax.rsqrt(row_var + norm_epsilon) * gain_vector


def contract(left, turned):
    return lax.dot_general(
        left, turned, (((1,), (1,)), ((), ())), preferred_element_type=jnp.float32
    )


def swap_blocks(x):
    return lax.all_to_all(x, "tp", 0, 0, tiled=True)


def summed(tiles):
    return jnp.sum(tiles.astype(jnp.float32), axis=0).astype(jnp.bfloat16)


def shards(
    stream,
    in_gain,
    value_weight,
    gate_weight,
    conv_kernel,
    conv_gain,
    conv_shift,
    out_weight,
    norm_gain,
    up_weight,
    down_weight,
    out_gain,
):
    seq_count, seq_length, model_width = stream.shape
    token_count = seq_count * seq_length
    tp_count = lax.axis_size("tp")
    group_count = lax.axis_size("grp")
    slice_width = model_width // tp_count
    own_tokens = token_count // tp_count
    tp_index = lax.axis_index("tp")
    channels = value_weight.shape[1]

    sharing = 2 if group_count % 2 == 0 else 1
    partner = [(g, g ^ 1) for g in range(group_count)]
    is_even = lax.axis_index("grp") % 2 == 0
    teams = [
        [g * tp_count + t for t in range(tp_count) for g in range(first, first + sharing)]
        for first in range(0, group_count, sharing)
    ]
    share = up_weight.shape[1] // sharing
    up_shard, down_shard = up_weight, down_weight.T
    if sharing == 2:
        up_shard = jnp.where(is_even, up_shard[:, :share], up_shard[:, share:])
        down_shard = jnp.where(is_even, down_shard[:, :share], down_shard[:, share:])
    feed = gather_fs(jnp.concatenate([up_shard, down_shard], axis=1))
    up_whole, down_turned = feed[:, :share], feed[:, share:]

    rows = value_weight.shape[0]
    half = rows // 2
    out_shard = out_weight.T
    even_part = jnp.concatenate([value_weight, out_shard[:half]], axis=0)
    odd_part = jnp.concatenate([gate_weight, out_shard[half:]], axis=0)
    if sharing == 2:
        mine = gather_in_strides(jnp.where(is_even, even_part, odd_part))
        theirs = lax.ppermute(mine, "grp", partner)
        even_whole, odd_whole = in_order(is_even, mine, theirs)
    else:
        even_whole, odd_whole = gather_fs(even_part), gather_fs(odd_part)
    even_whole = even_whole.reshape(-1, rows + half, channels)
    odd_whole = odd_whole.reshape(-1, rows + half, channels)
    value_whole = even_whole[:, :rows].reshape(-1, channels)
    gate_whole = odd_whole[:, :rows].reshape(-1, channels)
    out_turned = jnp.concatenate([even_whole[:, rows:], odd_whole[:, rows:]], axis=1).reshape(-1, channels)

    normed = norm_rows(
        stream.reshape(token_count, model_width).astype(jnp.float32), in_gain
    ).astype(jnp.bfloat16)
    values = jnp.dot(normed, value_whole, preferred_element_type=jnp.float32)
    gating = jnp.dot(normed, gate_whole, preferred_element_type=jnp.float32)
    gated = (values * jax.nn.sigmoid(gating)).astype(jnp.bfloat16)
    convolved = lax.conv_general_dilated(
        gated.reshape(seq_count, seq_length, channels),
        conv_kernel[:, None, :],
        window_strides=(1,),
        padding=[(KW - 1, 0)],
        dimension_numbers=("NWC", "WIO", "NWC"),
        feature_group_count=channels,
        preferred_element_type=jnp.float32,
    ).reshape(token_count, channels)
    told = jnp.concatenate(
        [jnp.sum(convolved, axis=1), jnp.sum(convolved * convolved, axis=1), out_gain]
    )
    normed_own = lax.dynamic_slice_in_dim(normed, tp_index * own_tokens, own_tokens, 0)
    told, out_turned, normed_own, norm_gain = lax.optimization_barrier(
        (told, out_turned, normed_own, norm_gain)
    )
    heard = swap_blocks(jnp.broadcast_to(told[None], (tp_count, *told.shape)))
    sums = jnp.sum(heard[:, : 2 * token_count], axis=0).reshape(2, token_count)
    whole_gain = heard[:, 2 * token_count :].reshape(model_width)
    row_mean = sums[0] / (channels * tp_count)
    row_var = sums[1] / (channels * tp_count) - row_mean * row_mean
    activated = jax.nn.silu(
        (convolved - row_mean[:, None]) * lax.rsqrt(row_var + norm_epsilon)[:, None] * conv_gain
        + conv_shift
    ).astype(jnp.bfloat16)

    mixed_terms = contract(activated, out_turned).astype(jnp.bfloat16)
    mixed_terms, whole_gain = lax.optimization_barrier((mixed_terms, whole_gain))
    mixed = summed(swap_blocks(mixed_terms.reshape(tp_count, own_tokens, model_width)))
    settled_own = norm_rows(
        residual_scale * normed_own.astype(jnp.float32) + mixed.astype(jnp.float32), norm_gain
    ).astype(jnp.bfloat16)
    if sharing == 2:
        their_settled = lax.ppermute(settled_own, "grp", partner)
        pair_settled = jnp.stack(in_order(is_even, settled_own, their_settled))
    else:
        pair_settled = settled_own[None]
    settled = from_half(
        lax.all_gather(to_half(pair_settled, feature_scale), "tp", axis=0, tiled=True),
        feature_scale,
    ).reshape(sharing * token_count, model_width)

    hidden = jnp.square(
        jax.nn.relu(jnp.dot(settled, up_whole, preferred_element_type=jnp.float32))
    ).astype(jnp.bfloat16)
    hidden = lax.optimization_barrier(hidden)
    fed_terms = contract(hidden, down_turned).astype(jnp.bfloat16)
    fed = summed(
        lax.all_to_all(
            fed_terms.reshape(sharing * tp_count, own_tokens, model_width),
            ("grp", "tp"),
            0,
            0,
            tiled=True,
            axis_index_groups=teams,
        )
    )
    result_own = norm_rows(
        residual_scale * settled_own.astype(jnp.float32) + fed.astype(jnp.float32), whole_gain
    ).astype(jnp.bfloat16)
    pieces = jnp.moveaxis(result_own.reshape(own_tokens, tp_count, slice_width), 1, 0)
    return swap_blocks(pieces).reshape(seq_count, seq_length, slice_width)


def solution(mesh):
    in_specs = (
        P(("grp", "fs"), None, None),
        P(),
        P("fs", "tp"),
        P("fs", "tp"),
        P(None, "tp"),
        P("tp"),
        P("tp"),
        P("tp", "fs"),
        P(),
        P("fs", "tp"),
        P("tp", "fs"),
        P("tp"),
    )
    out_specs = P(("grp", "fs"), None, "tp")
    return jax.shard_map(shards, mesh=mesh, in_specs=in_specs, out_specs=out_specs, check_vma=False)
```
